32 devices in a mesh: grp: 2 (over y), sp: 4 (over z), tp: 4 (over x, core).
Axes of the slice: x: 2, y: 2, z: 4, core: 2. Of those that a mesh axis runs over, the one named last changes fastest.
Arguments:
- hidden_in: bfloat16 [3072, 4096], P(('grp', 'sp'), 'tp'), parts along dimension 0, may hold values from -30 to 30
- in_gain: float32 [2, 4096], P(None, 'tp'), may hold values from 0.1 to 1.9
- w_value: bfloat16 [2, 4096, 2048], P(None, 'sp', 'tp'), may hold values from -0.09375 to 0.09375
- w_gate: bfloat16 [2, 4096, 2048], P(None, 'sp', 'tp'), may hold values from -0.09375 to 0.09375
- conv_taps: float32 [2, 31, 2048], P(None, None, 'tp'), may hold values from -9 to 9
- norm_gain: float32 [2, 2048], P(None, 'tp'), may hold values from 0.1 to 1.9
- norm_shift: float32 [2, 2048], P(None, 'tp'), may hold values from -3 to 3
- w_out: bfloat16 [2, 2048, 4096], P(None, 'tp', 'sp'), may hold values from -0.125 to 0.125
Outputs:
- hidden_out: bfloat16 [3072, 4096], P(('grp', 'sp'), 'tp'), parts along dimension 0
The draws below stay inside these ranges and needn't reach their ends.
There are 2 independent parts, one for each index of `grp`. The reference program is written for one: setup_inputs(seed, part) draws one part's arguments, and reference() takes and returns one part's arrays. A program takes and returns all parts, laid end to end along the dimension named above; an argument that names none is the same for every part. Nothing has to cross between parts.
All inputs are finite; a program needn't handle non-finite values.
Results may differ from the reference program's by a relative error of at most 0.013.
Values may be sent and summed in bfloat16 or wider, within the bound.
A program may use at most 64 MiB of HBM per device.

```python
import math
import jax
import jax.numpy as jnp
from jax import lax

D = 4096
C = 2048
KERNEL = 31
LAYERS = 2
TOKENS = 1536
N_TP = 4


def draw_hidden_in(key, part):
    keys = jax.random.split(key, 3)
    base = jnp.clip(jax.random.normal(keys[0], (TOKENS, D), jnp.float32), -4.0, 4.0)
    ramp = 3.0 ** (jnp.arange(D, dtype=jnp.float32) / D - 0.5)
    column = ramp * jnp.exp(jax.random.uniform(keys[1], (D,), jnp.float32, math.log(0.6), math.log(1.6)))
    row_scale = jnp.exp(jax.random.uniform(keys[2], (TOKENS,), jnp.float32, math.log(0.4), math.log(2.5)))
    return (base * row_scale[:, None] * column[None, :]).astype(jnp.bfloat16)


def draw_conv_taps(key, part):
    keys = jax.random.split(key, 2)
    base = jnp.clip(jax.random.normal(keys[0], (LAYERS, KERNEL, C), jnp.float32), -4.0, 4.0)
    ramp = 3.0 ** (jnp.arange(C, dtype=jnp.float32) / C)
    channel = ramp * jnp.exp(jax.random.uniform(keys[1], (C,), jnp.float32, 0.0, math.log(4.0)))
    return base / math.sqrt(KERNEL) * channel[None, None, :]


def block_levels(own_key, extent, pieces, smallest, largest):
    level, own = 1.0, jax.random.fold_in(own_key, 6)
    for axis_at, parts in pieces:
        heights = jnp.exp(jax.random.uniform(jax.random.fold_in(own, axis_at), (parts,), jnp.float32, smallest / len(pieces), largest / len(pieces)))
        level = level * jnp.repeat(heights, extent[axis_at] // parts).reshape([-1 if axis == axis_at else 1 for axis in range(len(extent))])
    return level


def scatter_about(own_key, shape, spread, most, cuts=(), kind=jnp.bfloat16):
    drawn = spread * jax.random.normal(own_key, shape, jnp.float32)
    if cuts:
        drawn = drawn * block_levels(own_key, shape, cuts, -0.22, 0.18)
    return jnp.clip(drawn, -most, most).astype(kind)


def setup_inputs(seed: int = 0, part: int = 0) -> dict:
    key_of = jax.random.split(jax.random.key(seed), 9)
    own_keys = jax.random.split(jax.random.fold_in(key_of[8], part), 9)
    return {
        "hidden_in": draw_hidden_in(jax.random.fold_in(jax.random.fold_in(key_of[8], part), 71), part),
        "in_gain": jnp.clip(1.0 + 0.18 * jax.random.normal(key_of[1], (LAYERS, D), jnp.float32), 0.1, 1.9),
        "w_value": scatter_about(key_of[2], (LAYERS, D, C), D ** -0.5, 0.09375, ((1, 4), (2, 4))),
        "w_gate": scatter_about(key_of[3], (LAYERS, D, C), D ** -0.5, 0.09375, ((1, 4), (2, 4))),
        "conv_taps": draw_conv_taps(jax.random.fold_in(key_of[8], 71), part),
        "norm_gain": jnp.clip(1.0 + 0.18 * jax.random.normal(key_of[5], (LAYERS, C), jnp.float32), 0.1, 1.9),
        "norm_shift": scatter_about(key_of[6], (LAYERS, C), 0.5, 3.0, ((1, 4),), jnp.float32),
        "w_out": scatter_about(key_of[7], (LAYERS, C, D), C ** -0.5, 0.125, ((1, 4), (2, 4))),
    }


epsilon = 1e-06

def block_sum(mixed_out, weight):
    block_width = C // N_TP

    def add_block(block_index, running):
        offset = block_index.astype(jnp.int32) * block_width
        block_cols = lax.dynamic_slice_in_dim(mixed_out, offset, block_width, 1)
        block_rows = lax.dynamic_slice_in_dim(weight, offset, block_width, 0)
        partial_value = jnp.dot(block_cols, block_rows, preferred_element_type=jnp.float32).astype(jnp.bfloat16)
        partial_value = lax.optimization_barrier(partial_value)
        return running + partial_value.astype(jnp.float32)
    start_sum = jnp.zeros((mixed_out.shape[0], weight.shape[1]), jnp.float32)
    return lax.fori_loop(0, N_TP, add_block, start_sum)

def causal_taps(gated_wide, taps):
    row_total = gated_wide.shape[0]
    padded = jnp.concatenate([jnp.zeros((KERNEL - 1, gated_wide.shape[1]), jnp.float32), gated_wide], axis=0)

    def add_tap(tap_index, running):
        where = tap_index.astype(jnp.int32)
        window = lax.dynamic_slice_in_dim(padded, where, row_total, 0)
        weight_row = lax.dynamic_slice_in_dim(taps, where, 1, 0)
        return running + weight_row * window
    start_sum = jnp.zeros(gated_wide.shape, jnp.float32)
    return lax.fori_loop(0, KERNEL, add_tap, start_sum)

def reference(hidden_in, in_gain, w_value, w_gate, conv_taps, norm_gain, norm_shift, w_out):
    hidden = hidden_in
    for layer_idx in range(LAYERS):
        widened = hidden.astype(jnp.float32)
        inv_rms = lax.rsqrt(lax.optimization_barrier(jnp.mean(widened * widened, axis=1, keepdims=True)) + epsilon)
        normalized = (widened * inv_rms * in_gain[layer_idx]).astype(jnp.bfloat16)
        value_part = jnp.dot(normalized, w_value[layer_idx], preferred_element_type=jnp.float32)
        gate_part = jnp.dot(normalized, w_gate[layer_idx], preferred_element_type=jnp.float32)
        gated = (value_part * jax.nn.sigmoid(gate_part)).astype(jnp.bfloat16)
        conved = causal_taps(gated.astype(jnp.float32), conv_taps[layer_idx])
        row_mean = lax.optimization_barrier(jnp.mean(conved, axis=1, keepdims=True))
        variance = lax.optimization_barrier(jnp.mean(jnp.square(conved - row_mean), axis=1, keepdims=True))
        normed = (conved - row_mean) * lax.rsqrt(variance + epsilon) * norm_gain[layer_idx] + norm_shift[layer_idx]
        mixed_out = jax.nn.silu(normed).astype(jnp.bfloat16)
        branch = block_sum(mixed_out, w_out[layer_idx])
        hidden = (hidden.astype(jnp.float32) + branch).astype(jnp.bfloat16)
    return hidden
```

```python
import jax
import jax.numpy as jnp
from jax import lax
from jax.sharding import PartitionSpec as P

epsilon = 1e-06


def passed_along(value, axis, steps):
    count = lax.axis_size(axis)
    initial, last = (max(0, -steps), min(count, count - steps))
    return lax.ppermute(value, axis, [(source, source + steps) for source in range(initial, last)])


def depthwise(extended, kernel_taps):
    conved = lax.conv_general_dilated(
        extended.astype(jnp.float32)[None],
        kernel_taps[:, None, :],
        (1,),
        [(0, 0)],
        dimension_numbers=("NWC", "WIO", "NWC"),
        feature_group_count=extended.shape[1],
        precision=lax.Precision.HIGHEST,
    )
    return conved[0]


def whole(shard):
    count, line = lax.axis_size("sp"), lax.axis_index("sp")
    lines = lax.axis_size("grp")
    mine = lax.axis_index("grp")
    halves = shard.reshape(lines, shard.shape[0] // lines, shard.shape[1])
    part = lax.dynamic_index_in_dim(halves, mine, 0, keepdims=False)
    full = jnp.zeros((count,) + halves.shape, shard.dtype)
    full = lax.dynamic_update_slice(full, halves[None], (line, 0, 0, 0))
    from_left, from_right = part, part
    rights, lefts = [], []
    for step in range(1, count):
        from_left = lax.ppermute(from_left, "sp", [(s, s + 1) for s in range(step - 1, count - 1)])
        from_right = lax.ppermute(from_right, "sp", [(s, s - 1) for s in range(1, count - step + 1)])
        rights.append(from_left)
        lefts.append(from_right)
    for slot in range(1, count):
        owner = lax.rem(line + slot, count)
        block = jnp.where(line + slot < count, lefts[slot - 1], rights[count - slot - 1])
        full = lax.dynamic_update_slice(full, block[None, None], (owner, mine, 0, 0))
        for shift in range(1, lines):
            other = lax.ppermute(block, "grp", [(s, (s + shift) % lines) for s in range(lines)])
            full = lax.dynamic_update_slice(
                full, other[None, None], (owner, lax.rem(mine + lines - shift, lines), 0, 0)
            )
    return full.reshape(count, *shard.shape)


def shards(hidden_in, in_gain, w_value, w_gate, conv_taps, norm_gain, norm_shift, w_out):
    layer_count = w_value.shape[0]
    reach_rows = conv_taps.shape[1] - 1
    features = hidden_in.shape[1] * lax.axis_size("tp")
    channels = w_value.shape[2] * lax.axis_size("tp")
    weights = []
    for layer_idx in range(layer_count):
        pair = jnp.concatenate([w_value[layer_idx], w_gate[layer_idx]], axis=1)
        weights.append((whole(pair), whole(w_out[layer_idx])))
    current = hidden_in
    for layer_idx in range(layer_count):
        pair_all, out_all = weights[layer_idx]
        pair_all = pair_all.reshape(features, -1)
        widened = current.astype(jnp.float32)
        squares = lax.psum(jnp.sum(widened * widened, axis=1), "tp")
        normalized = (
            widened * lax.rsqrt(squares / features + epsilon)[:, None] * in_gain[layer_idx]
        ).astype(jnp.bfloat16)
        gathered = lax.all_gather(normalized, "tp", axis=1, tiled=True)
        both = jnp.dot(gathered, pair_all, preferred_element_type=jnp.float32)
        value_part, gate_part = jnp.split(both, 2, axis=1)
        gated = (value_part * jax.nn.sigmoid(gate_part)).astype(jnp.bfloat16)
        before = passed_along(gated[gated.shape[0] - reach_rows :], "sp", 1)
        extended = jnp.concatenate([before, gated], axis=0)
        residual = current
        conved = depthwise(extended, conv_taps[layer_idx])
        total_sum, total_squares = lax.psum(
            (jnp.sum(conved, axis=1), jnp.sum(conved * conved, axis=1)), "tp"
        )
        row_mean = total_sum / channels
        spread = total_squares / channels - row_mean * row_mean
        normed = (conved - row_mean[:, None]) * lax.rsqrt(spread + epsilon)[:, None] * norm_gain[
            layer_idx
        ] + norm_shift[layer_idx]
        mixed_out = jax.nn.silu(normed).astype(jnp.bfloat16)
        partial_value = jnp.concatenate(
            [
                jnp.dot(mixed_out, out_all[block], preferred_element_type=jnp.float32).astype(jnp.bfloat16)
                for block in range(out_all.shape[0])
            ],
            axis=1,
        )
        summed = lax.psum_scatter(partial_value, "tp", scatter_dimension=1, tiled=True).astype(jnp.float32)
        current = (residual.astype(jnp.float32) + summed).astype(jnp.bfloat16)
    return current


def solution(mesh):
    placed = (
        P(("grp", "sp"), "tp"),
        P(None, "tp"),
        P(None, "sp", "tp"),
        P(None, "sp", "tp"),
        P(None, None, "tp"),
        P(None, "tp"),
        P(None, "tp"),
        P(None, "tp", "sp"),
    )
    return jax.shard_map(
        shards, mesh=mesh, in_specs=placed, out_specs=P(("grp", "sp"), "tp"), check_vma=False
    )
```

```python
import functools

import jax
import jax.numpy as jnp
from jax import lax
from jax.experimental import pallas as pl
from jax.experimental.pallas import tpu as pltpu
from jax.sharding import PartitionSpec as P

epsilon = 1e-06
CHUNK = 128
F32, BF16 = jnp.float32, jnp.bfloat16


def kernel(
    S, T, h_ref, gain_ref, wv_ref, wg_ref, taps_ref, ng_ref, ns_ref, wo_ref, out_ref,
    WV, WG, WO, X, ACC, EXT, CONV, MIX, PART, PRECV, SUMB, RECV, STAT, HB,
    own_sem, zr, zs_right, zs_left, yr, ys, xr, xs, xf, sr, ss, hr, hs, pr, ps, rr, rs,
):
    L = wv_ref.shape[0]
    Ds, Cn = wv_ref.shape[1], wv_ref.shape[2]
    rows, Dt = h_ref.shape
    taps = taps_ref.shape[1]
    features, channels = Dt * T, Cn * T
    chips = T // 2
    halo = EXT.shape[1] - rows
    g, me, t = lax.axis_index("grp"), lax.axis_index("sp"), lax.axis_index("tp")
    core = lax.rem(t, 2)
    chip = lax.div(t, 2)
    partner = t + 1 - 2 * core
    MESH = pl.DeviceIdType.MESH
    first, last = me == 0, me == S - 1

    sources = [(wv_ref, WV), (wg_ref, WG), (wo_ref, WO)]

    def own(layer, which):
        source, slots = sources[which]
        return pltpu.make_async_copy(source.at[layer], slots.at[layer, me], own_sem.at[layer, which])

    for layer in range(L):
        for which in range(3):
            own(layer, which).start()

    def each_chunk(body, size=CHUNK):
        def step(index, _):
            body(pl.ds(pl.multiple_of(index * size, size), size))
            return 0

        lax.fori_loop(0, rows // size, step, 0)

    def put_stat(slot, where, left, right):
        lane = lax.broadcasted_iota(jnp.int32, (left.shape[0], 128), 1)
        wide = jnp.where(lane == 0, left, right)
        STAT[slot, t, :, where] = wide.T[:8]

    def stat_copy(slot, peer):
        return pltpu.make_async_remote_copy(
            STAT.at[slot, t], STAT.at[slot, t], ss.at[slot, peer], sr.at[slot, t],
            device_id={"tp": peer}, device_id_type=MESH,
        )

    def stat_arrival(slot, peer):
        return pltpu.make_async_remote_copy(
            STAT.at[slot, peer], STAT.at[slot, peer], ss.at[slot, peer], sr.at[slot, peer],
            device_id={"tp": peer}, device_id_type=MESH,
        )

    def send_stat(slot):
        for shift in range(1, T):
            stat_copy(slot, lax.rem(t + shift, T)).start()

    def wait_stat(slot):
        for shift in range(1, T):
            stat_arrival(slot, lax.rem(t + shift, T)).wait_recv()

    def get_stat(slot, where):
        total = STAT[slot, 0, :, where]
        for peer in range(1, T):
            total = total + STAT[slot, peer, :, where]
        return jnp.concatenate([total] * 16, axis=0).T

    def half_ref(item, owner):
        kind, layer = item % 4, item // 4
        if kind < 2:
            size = Ds // 2
            return (WV, WG)[kind].at[layer, owner, pl.ds(pl.multiple_of(g * size, size), size)]
        size = Cn // 4
        start = pl.multiple_of(g * (2 * size) + (kind - 2) * size, size)
        return WO.at[layer, owner, pl.ds(start, size)]

    def other_ref(item, owner):
        kind, layer = item % 4, item // 4
        if kind < 2:
            size = Ds // 2
            return (WV, WG)[kind].at[layer, owner, pl.ds(pl.multiple_of((1 - g) * size, size), size)]
        size = Cn // 4
        start = pl.multiple_of((1 - g) * (2 * size) + (kind - 2) * size, size)
        return WO.at[layer, owner, pl.ds(start, size)]

    def zcopy(item, owner, way):
        ref = half_ref(item, owner)
        sems = zs_right if way > 0 else zs_left
        return pltpu.make_async_remote_copy(
            ref, ref, sems.at[item, owner], zr.at[item, owner],
            device_id={"sp": me + way}, device_id_type=MESH,
        )

    def ycopy(item, owner):
        ref = half_ref(item, owner)
        return pltpu.make_async_remote_copy(
            ref, ref, ys.at[item, owner], yr.at[item, owner],
            device_id={"grp": 1 - g}, device_id_type=MESH,
        )

    def yarrival(item, owner):
        ref = other_ref(item, owner)
        return pltpu.make_async_remote_copy(
            ref, ref, ys.at[item, owner], yr.at[item, owner],
            device_id={"grp": 1 - g}, device_id_type=MESH,
        )

    def event(item, k):
        if k == 0:
            if item % 4 < 3:
                own(item // 4, item % 4).wait()

            @pl.when(jnp.logical_not(last))
            def _():
                zcopy(item, me, 1).start()

            @pl.when(jnp.logical_not(first))
            def _():
                zcopy(item, me, -1).start()

            return

        @pl.when(me - k >= 0)
        def _():
            owner = me - k
            zcopy(item, owner, 1).wait_recv()

            @pl.when(jnp.logical_not(last))
            def _():
                zcopy(item, owner, 1).start()

            ycopy(item, owner).start()

        @pl.when(me + k < S)
        def _():
            owner = me + k
            zcopy(item, owner, -1).wait_recv()

            @pl.when(jnp.logical_not(first))
            def _():
                zcopy(item, owner, -1).start()

            ycopy(item, owner).start()

    def xcopy(layer, source, peer, sem):
        return pltpu.make_async_remote_copy(
            X.at[layer, source], X.at[layer, source], sem, xr.at[layer, source],
            device_id={"tp": peer}, device_id_type=MESH,
        )

    def make_x(layer):
        source = h_ref if layer == 0 else HB

        def body(where):
            wide = source[where, :].astype(F32)
            X[layer, t, where, :] = (wide * gain_ref[layer : layer + 1, :]).astype(BF16)
            squares = jnp.sum(wide * wide, axis=1, keepdims=True)
            put_stat(2 * layer, where, squares, squares)

        each_chunk(body)

    def send_x(layer):
        for shift in range(1, chips):
            peer = lax.rem(chip + shift, chips) * 2 + core
            xcopy(layer, t, peer, xs.at[layer, shift]).start()
        xcopy(layer, t, partner, xs.at[layer, 0]).start()
        send_stat(2 * layer)

    def relay_x(layer):
        for shift in range(1, chips):
            source = lax.rem(chip + shift, chips) * 2 + core
            xcopy(layer, source, partner, xf.at[layer, shift]).wait_recv()
            xcopy(layer, source, partner, xf.at[layer, shift]).start()

    def wait_x(layer):
        for shift in range(chips):
            source = lax.rem(chip + shift, chips) * 2 + 1 - core
            xcopy(layer, source, partner, xf.at[layer, 0]).wait_recv()
        wait_stat(2 * layer)

    def project(layer):
        def block(owner, _):
            @pl.when(owner != me)
            def _():
                yarrival(4 * layer, owner).wait_recv()
                yarrival(4 * layer + 1, owner).wait_recv()

            at = lax.div(owner * Ds, Dt)
            columns = pl.ds(pl.multiple_of(lax.rem(owner * Ds, Dt), 128), Ds)
            xs_block = X[layer, at, :, columns]
            for which, slots in ((0, WV), (1, WG)):
                part = jnp.dot(xs_block, slots[layer, owner], preferred_element_type=F32)

                @pl.when(owner == 0)
                def _():
                    ACC[which] = part

                @pl.when(owner > 0)
                def _():
                    ACC[which] += part

            return 0

        lax.fori_loop(0, S, block, 0)

    def halo_copy(layer):
        return pltpu.make_async_remote_copy(
            EXT.at[layer, pl.ds(rows, halo)], EXT.at[layer, pl.ds(0, halo)], hs.at[layer], hr.at[layer],
            device_id={"sp": me + 1}, device_id_type=MESH,
        )

    def gate(layer):
        def body(where):
            mean = get_stat(2 * layer, where)[:, :1] / features
            inv = lax.rsqrt(mean + epsilon)
            value, gating = ACC[0, where, :] * inv, ACC[1, where, :] * inv
            gated = (value / (1.0 + jnp.exp(-gating))).astype(BF16).astype(F32)
            EXT[layer, pl.ds(pl.multiple_of(where.start + halo, 8), where.size), :] = gated

        each_chunk(body)

        @pl.when(jnp.logical_not(last))
        def _():
            halo_copy(layer).start()

        @pl.when(first)
        def _():
            EXT[layer, pl.ds(0, halo), :] = jnp.zeros((halo, Cn), F32)

    def convolve(layer):
        @pl.when(jnp.logical_not(first))
        def _():
            halo_copy(layer).wait_recv()

        tall = CHUNK + halo + 8
        offset = halo - (taps - 1)

        def body(where):
            for column in range(0, Cn, 128):
                at = pl.ds(column, 128)
                tile = jnp.concatenate(
                    [EXT[layer, pl.ds(where.start, CHUNK + halo), at], jnp.zeros((8, 128), F32)], axis=0
                )
                total = jnp.zeros((CHUNK, 128), F32)
                for residue in range(8):
                    ks = [k for k in range(taps) if (k + offset) % 8 == residue]
                    if not ks:
                        continue
                    turned = pltpu.roll(tile, tall - residue, 0) if residue else tile
                    for k in ks:
                        low = k + offset - residue
                        total = total + taps_ref[layer, k : k + 1, at] * turned[low : low + CHUNK]
                CONV[where, at] = total
            conved = CONV[where, :]
            put_stat(
                2 * layer + 1, where,
                jnp.sum(conved, axis=1, keepdims=True),
                jnp.sum(conved * conved, axis=1, keepdims=True),
            )

        each_chunk(body)
        send_stat(2 * layer + 1)

    def mix(layer):
        wait_stat(2 * layer + 1)

        def body(where):
            stat = get_stat(2 * layer + 1, where)
            mean = stat[:, 0:1] / channels
            spread = stat[:, 1:2] / channels - mean * mean
            normed = (CONV[where, :] - mean) * lax.rsqrt(spread + epsilon) * ng_ref[
                layer : layer + 1, :
            ] + ns_ref[layer : layer + 1, :]
            MIX[where, :] = (normed / (1.0 + jnp.exp(-normed))).astype(BF16)

        each_chunk(body)

    def pair_copy(layer, at):
        return pltpu.make_async_remote_copy(
            PART.at[layer, 2 * at + 1 - core], PRECV.at[layer, at], ps.at[layer, at], pr.at[layer, at],
            device_id={"tp": partner}, device_id_type=MESH,
        )

    def sum_copy(layer, at):
        return pltpu.make_async_remote_copy(
            SUMB.at[layer, at], RECV.at[layer, chip], rs.at[layer, at], rr.at[layer, chip],
            device_id={"tp": at * 2 + core}, device_id_type=MESH,
        )

    def sum_arrival(layer, at):
        return pltpu.make_async_remote_copy(
            SUMB.at[layer, at], RECV.at[layer, at], rs.at[layer, at], rr.at[layer, at],
            device_id={"tp": at * 2 + core}, device_id_type=MESH,
        )

    def branch(layer):
        def block(owner, _):
            @pl.when(owner != me)
            def _():
                yarrival(4 * layer + 2, owner).wait_recv()
                yarrival(4 * layer + 3, owner).wait_recv()

            at = lax.div(owner * Ds, Dt)
            columns = pl.ds(pl.multiple_of(lax.rem(owner * Ds, Dt), 128), Ds)
            PART[layer, at, :, columns] = jnp.dot(
                MIX[...], WO[layer, owner], preferred_element_type=F32
            ).astype(BF16)
            return 0

        lax.fori_loop(0, S, block, 0)
        for shift in list(range(1, chips)) + [0]:
            pair_copy(layer, lax.rem(chip + shift, chips)).start()

    def reduce_pairs(layer):
        for shift in range(1, chips):
            at = lax.rem(chip + shift, chips)
            pair_copy(layer, at).wait_recv()

            def body(where, at=at):
                SUMB[layer, at, where, :] = (
                    PART[layer, at * 2 + core, where, :].astype(F32) + PRECV[layer, at, where, :].astype(F32)
                ).astype(BF16)

            each_chunk(body)
            sum_copy(layer, at).start()

    def finish(layer):
        pair_copy(layer, chip).wait_recv()
        for shift in range(1, chips):
            sum_arrival(layer, lax.rem(chip + shift, chips)).wait_recv()
        source = h_ref if layer == 0 else HB
        target = out_ref if layer == L - 1 else HB

        def body(where):
            total = PART[layer, t, where, :].astype(F32) + PRECV[layer, chip, where, :].astype(F32)
            for shift in range(1, chips):
                total = total + RECV[layer, lax.rem(chip + shift, chips), where, :].astype(F32)
            target[where, :] = (source[where, :].astype(F32) + total).astype(BF16)

        each_chunk(body)

    make_x(0)
    barrier = pltpu.get_barrier_semaphore()
    for shift in range(1, T):
        pl.semaphore_signal(barrier, inc=1, device_id={"tp": lax.rem(t + shift, T)}, device_id_type=MESH)
    pl.semaphore_signal(barrier, inc=1, device_id={"grp": 1 - g}, device_id_type=MESH)

    @pl.when(jnp.logical_not(first))
    def _():
        pl.semaphore_signal(barrier, inc=1, device_id={"sp": me - 1}, device_id_type=MESH)

    @pl.when(jnp.logical_not(last))
    def _():
        pl.semaphore_signal(barrier, inc=1, device_id={"sp": me + 1}, device_id_type=MESH)

    inner = jnp.where(first, 0, 1) + jnp.where(last, 0, 1)
    pl.semaphore_wait(barrier, T + inner)

    event(0, 0)
    event(1, 0)
    send_x(0)

    def pumped(items, stages):
        for k in range(1, S):
            for item in items:
                event(item, k)
            if stages:
                stages.pop(0)()
        for stage in stages:
            stage()

    stages = [functools.partial(relay_x, 0), functools.partial(wait_x, 0)]
    for layer in range(L):
        base = 4 * layer
        pumped([base, base + 1], stages)
        event(base + 2, 0)
        event(base + 3, 0)
        if layer + 1 < L:
            event(base + 4, 0)
        project(layer)
        gate(layer)
        pumped(
            [base + 2, base + 3],
            [functools.partial(convolve, layer), functools.partial(mix, layer)],
        )
        if layer + 1 < L:
            event(base + 5, 0)
        branch(layer)
        if layer + 1 < L:

            def next_x(layer=layer):
                finish(layer)
                make_x(layer + 1)
                send_x(layer + 1)

            def arrive_x(layer=layer):
                relay_x(layer + 1)
                wait_x(layer + 1)

            reduce_pairs(layer)
            stages = [next_x, arrive_x]
        else:
            reduce_pairs(layer)
            finish(layer)

    for item in range(4 * L):

        def drain(owner, _, item=item):
            @pl.when(jnp.logical_and(owner <= me, jnp.logical_not(last)))
            def _():
                zcopy(item, owner, 1).wait_send()

            @pl.when(jnp.logical_and(owner >= me, jnp.logical_not(first)))
            def _():
                zcopy(item, owner, -1).wait_send()

            @pl.when(owner != me)
            def _():
                ycopy(item, owner).wait_send()

            return 0

        lax.fori_loop(0, S, drain, 0)
    for layer in range(L):
        for slot in (2 * layer, 2 * layer + 1):
            for shift in range(1, T):
                stat_copy(slot, lax.rem(t + shift, T)).wait_send()
        for shift in range(chips):
            xcopy(layer, t, partner, xs.at[layer, shift]).wait_send()
            pair_copy(layer, lax.rem(chip + shift, chips)).wait_send()
        for shift in range(1, chips):
            xcopy(layer, t, partner, xf.at[layer, shift]).wait_send()
            sum_copy(layer, lax.rem(chip + shift, chips)).wait_send()

        @pl.when(jnp.logical_not(last))
        def _(layer=layer):
            halo_copy(layer).wait_send()


def shards(hidden_in, in_gain, w_value, w_gate, conv_taps, norm_gain, norm_shift, w_out):
    S, T = lax.axis_size("sp"), lax.axis_size("tp")
    L, Ds, Cn = w_value.shape
    rows, Dt = hidden_in.shape
    chips = T // 2
    halo = (conv_taps.shape[1] - 1 + 7) // 8 * 8
    vmem = pl.BlockSpec(memory_space=pltpu.VMEM)
    hbm = pl.BlockSpec(memory_space=pl.ANY)
    dma = pltpu.SemaphoreType.DMA
    return pl.pallas_call(
        functools.partial(kernel, S, T),
        out_shape=jax.ShapeDtypeStruct((rows, Dt), BF16),
        in_specs=[vmem, vmem, hbm, hbm, vmem, vmem, vmem, hbm],
        out_specs=vmem,
        scratch_shapes=[
            pltpu.VMEM((L, S, Ds, Cn), BF16),
            pltpu.VMEM((L, S, Ds, Cn), BF16),
            pltpu.VMEM((L, S, Cn, Ds), BF16),
            pltpu.VMEM((L, T, rows, Dt), BF16),
            pltpu.VMEM((2, rows, Cn), F32),
            pltpu.VMEM((L, rows + halo, Cn), F32),
            pltpu.VMEM((rows, Cn), F32),
            pltpu.VMEM((rows, Cn), BF16),
            pltpu.VMEM((L, T, rows, Dt), BF16),
            pltpu.VMEM((L, chips, rows, Dt), BF16),
            pltpu.VMEM((L, chips, rows, Dt), BF16),
            pltpu.VMEM((L, chips, rows, Dt), BF16),
            pltpu.VMEM((2 * L, T, 8, rows), F32),
            pltpu.VMEM((rows, Dt), BF16),
            dma((L, 3)),
            dma((4 * L, S)), dma((4 * L, S)), dma((4 * L, S)), dma((4 * L, S)), dma((4 * L, S)),
            dma((L, T)), dma((L, chips)), dma((L, chips)),
            dma((2 * L, T)), dma((2 * L, T)),
            dma((L,)), dma((L,)),
            dma((L, chips)), dma((L, chips)),
            dma((L, chips)), dma((L, chips)),
        ],
        compiler_params=pltpu.CompilerParams(
            collective_id=0, has_side_effects=True, vmem_limit_bytes=64_000_000
        ),
    )(hidden_in, in_gain, w_value, w_gate, conv_taps, norm_gain, norm_shift, w_out)


def solution(mesh):
    placed = (
        P(("grp", "sp"), "tp"),
        P(None, "tp"),
        P(None, "sp", "tp"),
        P(None, "sp", "tp"),
        P(None, None, "tp"),
        P(None, "tp"),
        P(None, "tp"),
        P(None, "tp", "sp"),
    )
    return jax.shard_map(
        shards, mesh=mesh, in_specs=placed, out_specs=P(("grp", "sp"), "tp"), check_vma=False
    )
```

```python
import functools

import jax
import jax.numpy as jnp
from jax import lax
from jax.experimental import pallas as pl
from jax.experimental.pallas import tpu as pltpu
from jax.sharding import PartitionSpec as P

epsilon = 1e-06
CHUNK = 128
F32, BF16 = jnp.float32, jnp.bfloat16


def kernel(
    S, T, h_ref, gain_ref, wv_ref, wg_ref, taps_ref, ng_ref, ns_ref, wo_ref, out_ref,
    WV, WG, WO, X, ACC, EXT, CONV, MIX, PART, PRECV, SUMB, RECV, STAT, HB,
    own_sem, zr, zs_right, zs_left, yr, ys, xr, xs, xf, sr, ss, hr, hs, pr, ps, rr, rs,
):
    L = wv_ref.shape[0]
    Ds, Cn = wv_ref.shape[1], wv_ref.shape[2]
    rows, Dt = h_ref.shape
    taps = taps_ref.shape[1]
    features, channels = Dt * T, Cn * T
    chips = T // 2
    halo = EXT.shape[1] - rows
    g, me, t = lax.axis_index("grp"), lax.axis_index("sp"), lax.axis_index("tp")
    core = lax.rem(t, 2)
    chip = lax.div(t, 2)
    partner = t + 1 - 2 * core
    MESH = pl.DeviceIdType.MESH
    first, last = me == 0, me == S - 1

    sources = [(wv_ref, WV), (wg_ref, WG), (wo_ref, WO)]

    def own(layer, which):
        source, slots = sources[which]
        return pltpu.make_async_copy(source.at[layer], slots.at[layer, me], own_sem.at[layer, which])

    for layer in range(L):
        for which in range(3):
            own(layer, which).start()

    def each_chunk(body, size=CHUNK):
        def step(index, _):
            body(pl.ds(pl.multiple_of(index * size, size), size))
            return 0

        lax.fori_loop(0, rows // size, step, 0)

    def put_stat(slot, where, left, right):
        lane = lax.broadcasted_iota(jnp.int32, (left.shape[0], 128), 1)
        wide = jnp.where(lane == 0, left, right)
        STAT[slot, t, :, where] = wide.T[:8]

    def stat_copy(slot, peer):
        return pltpu.make_async_remote_copy(
            STAT.at[slot, t], STAT.at[slot, t], ss.at[slot, peer], sr.at[slot, t],
            device_id={"tp": peer}, device_id_type=MESH,
        )

    def stat_arrival(slot, peer):
        return pltpu.make_async_remote_copy(
            STAT.at[slot, peer], STAT.at[slot, peer], ss.at[slot, peer], sr.at[slot, peer],
            device_id={"tp": peer}, device_id_type=MESH,
        )

    def send_stat(slot):
        for shift in range(1, T):
            stat_copy(slot, lax.rem(t + shift, T)).start()

    def wait_stat(slot):
        for shift in range(1, T):
            stat_arrival(slot, lax.rem(t + shift, T)).wait_recv()

    def get_stat(slot, where):
        total = STAT[slot, 0, :, where]
        for peer in range(1, T):
            total = total + STAT[slot, peer, :, where]
        return jnp.concatenate([total] * 16, axis=0).T

    def half_ref(item, owner):
        kind, layer = item % 4, item // 4
        if kind < 2:
            size = Ds // 2
            return (WV, WG)[kind].at[layer, owner, pl.ds(pl.multiple_of(g * size, size), size)]
        size = Cn // 4
        start = pl.multiple_of(g * (2 * size) + (kind - 2) * size, size)
        return WO.at[layer, owner, pl.ds(start, size)]

    def other_ref(item, owner):
        kind, layer = item % 4, item // 4
        if kind < 2:
            size = Ds // 2
            return (WV, WG)[kind].at[layer, owner, pl.ds(pl.multiple_of((1 - g) * size, size), size)]
        size = Cn // 4
        start = pl.multiple_of((1 - g) * (2 * size) + (kind - 2) * size, size)
        return WO.at[layer, owner, pl.ds(start, size)]

    def zcopy(item, owner, way):
        ref = half_ref(item, owner)
        sems = zs_right if way > 0 else zs_left
        return pltpu.make_async_remote_copy(
            ref, ref, sems.at[item, owner], zr.at[item, owner],
            device_id={"sp": me + way}, device_id_type=MESH,
        )

    def ycopy(item, owner):
        ref = half_ref(item, owner)
        return pltpu.make_async_remote_copy(
            ref, ref, ys.at[item, owner], yr.at[item, owner],
            device_id={"grp": 1 - g}, device_id_type=MESH,
        )

    def yarrival(item, owner):
        ref = other_ref(item, owner)
        return pltpu.make_async_remote_copy(
            ref, ref, ys.at[item, owner], yr.at[item, owner],
            device_id={"grp": 1 - g}, device_id_type=MESH,
        )

    def event(item, k):
        if k == 0:
            if item % 4 < 3:
                own(item // 4, item % 4).wait()

            @pl.when(jnp.logical_not(last))
            def _():
                zcopy(item, me, 1).start()

            @pl.when(jnp.logical_not(first))
            def _():
                zcopy(item, me, -1).start()

            return

        @pl.when(me - k >= 0)
        def _():
            owner = me - k
            zcopy(item, owner, 1).wait_recv()

            @pl.when(jnp.logical_not(last))
            def _():
                zcopy(item, owner, 1).start()

            ycopy(item, owner).start()

        @pl.when(me + k < S)
        def _():
            owner = me + k
            zcopy(item, owner, -1).wait_recv()

            @pl.when(jnp.logical_not(first))
            def _():
                zcopy(item, owner, -1).start()

            ycopy(item, owner).start()

    def xcopy(layer, source, peer, sem):
        return pltpu.make_async_remote_copy(
            X.at[layer, source], X.at[layer, source], sem, xr.at[layer, source],
            device_id={"tp": peer}, device_id_type=MESH,
        )

    def make_x(layer):
        source = h_ref if layer == 0 else HB

        def body(where):
            wide = source[where, :].astype(F32)
            X[layer, t, where, :] = (wide * gain_ref[layer : layer + 1, :]).astype(BF16)
            squares = jnp.sum(wide * wide, axis=1, keepdims=True)
            put_stat(2 * layer, where, squares, squares)

        each_chunk(body)

    def send_x(layer):
        for shift in range(1, chips):
            peer = lax.rem(chip + shift, chips) * 2 + core
            xcopy(layer, t, peer, xs.at[layer, shift]).start()
        xcopy(layer, t, partner, xs.at[layer, 0]).start()
        send_stat(2 * layer)

    def relay_x(layer):
        for shift in range(1, chips):
            source = lax.rem(chip + shift, chips) * 2 + core
            xcopy(layer, source, partner, xf.at[layer, shift]).wait_recv()
            xcopy(layer, source, partner, xf.at[layer, shift]).start()

    def wait_x(layer):
        for shift in range(chips):
            source = lax.rem(chip + shift, chips) * 2 + 1 - core
            xcopy(layer, source, partner, xf.at[layer, 0]).wait_recv()
        wait_stat(2 * layer)

    def by_arrival(body):
        def step(turn, _):
            away = lax.div(turn + 1, 2)
            owner = jnp.where(lax.rem(turn, 2) == 1, me + away, me - away)

            @pl.when(jnp.logical_and(owner >= 0, owner < S))
            def _():
                body(turn, owner)

            return 0

        lax.fori_loop(0, 2 * S - 1, step, 0)

    def project(layer):
        def block(turn, owner):
            @pl.when(turn > 0)
            def _():
                yarrival(4 * layer, owner).wait_recv()
                yarrival(4 * layer + 1, owner).wait_recv()

            at = lax.div(owner * Ds, Dt)
            columns = pl.ds(pl.multiple_of(lax.rem(owner * Ds, Dt), 128), Ds)
            xs_block = X[layer, at, :, columns]
            for which, slots in ((0, WV), (1, WG)):
                part = jnp.dot(xs_block, slots[layer, owner], preferred_element_type=F32)

                @pl.when(turn == 0)
                def _():
                    ACC[which] = part

                @pl.when(turn > 0)
                def _():
                    ACC[which] += part

        by_arrival(block)

    def halo_copy(layer):
        return pltpu.make_async_remote_copy(
            EXT.at[layer, pl.ds(rows, halo)], EXT.at[layer, pl.ds(0, halo)], hs.at[layer], hr.at[layer],
            device_id={"sp": me + 1}, device_id_type=MESH,
        )

    def gate(layer):
        def body(where):
            mean = get_stat(2 * layer, where)[:, :1] / features
            inv = lax.rsqrt(mean + epsilon)
            value, gating = ACC[0, where, :] * inv, ACC[1, where, :] * inv
            gated = (value / (1.0 + jnp.exp(-gating))).astype(BF16).astype(F32)
            EXT[layer, pl.ds(pl.multiple_of(where.start + halo, 8), where.size), :] = gated

        each_chunk(body)

        @pl.when(jnp.logical_not(last))
        def _():
            halo_copy(layer).start()

        @pl.when(first)
        def _():
            EXT[layer, pl.ds(0, halo), :] = jnp.zeros((halo, Cn), F32)

    def convolve(layer):
        @pl.when(jnp.logical_not(first))
        def _():
            halo_copy(layer).wait_recv()

        tall = CHUNK + halo + 8
        offset = halo - (taps - 1)

        def body(where):
            for column in range(0, Cn, 128):
                at = pl.ds(column, 128)
                tile = jnp.concatenate(
                    [EXT[layer, pl.ds(where.start, CHUNK + halo), at], jnp.zeros((8, 128), F32)], axis=0
                )
                total = jnp.zeros((CHUNK, 128), F32)
                for residue in range(8):
                    ks = [k for k in range(taps) if (k + offset) % 8 == residue]
                    if not ks:
                        continue
                    turned = pltpu.roll(tile, tall - residue, 0) if residue else tile
                    for k in ks:
                        low = k + offset - residue
                        total = total + taps_ref[layer, k : k + 1, at] * turned[low : low + CHUNK]
                CONV[where, at] = total
            conved = CONV[where, :]
            put_stat(
                2 * layer + 1, where,
                jnp.sum(conved, axis=1, keepdims=True),
                jnp.sum(conved * conved, axis=1, keepdims=True),
            )

        each_chunk(body)
        send_stat(2 * layer + 1)

    def mix(layer):
        wait_stat(2 * layer + 1)

        def body(where):
            stat = get_stat(2 * layer + 1, where)
            mean = stat[:, 0:1] / channels
            spread = stat[:, 1:2] / channels - mean * mean
            normed = (CONV[where, :] - mean) * lax.rsqrt(spread + epsilon) * ng_ref[
                layer : layer + 1, :
            ] + ns_ref[layer : layer + 1, :]
            MIX[where, :] = (normed / (1.0 + jnp.exp(-normed))).astype(BF16)

        each_chunk(body)

    def pair_copy(layer, at):
        return pltpu.make_async_remote_copy(
            PART.at[layer, 2 * at + 1 - core], PRECV.at[layer, at], ps.at[layer, at], pr.at[layer, at],
            device_id={"tp": partner}, device_id_type=MESH,
        )

    def sum_copy(layer, at):
        return pltpu.make_async_remote_copy(
            SUMB.at[layer, at], RECV.at[layer, chip], rs.at[layer, at], rr.at[layer, chip],
            device_id={"tp": at * 2 + core}, device_id_type=MESH,
        )

    def sum_arrival(layer, at):
        return pltpu.make_async_remote_copy(
            SUMB.at[layer, at], RECV.at[layer, at], rs.at[layer, at], rr.at[layer, at],
            device_id={"tp": at * 2 + core}, device_id_type=MESH,
        )

    def sum_pair(layer, at):
        pair_copy(layer, at).wait_recv()

        def body(where):
            SUMB[layer, at, where, :] = (
                PART[layer, at * 2 + core, where, :].astype(F32) + PRECV[layer, at, where, :].astype(F32)
            ).astype(BF16)

        each_chunk(body)
        sum_copy(layer, at).start()

    def branch(layer):
        def block(turn, owner):
            @pl.when(turn > 0)
            def _():
                yarrival(4 * layer + 2, owner).wait_recv()
                yarrival(4 * layer + 3, owner).wait_recv()

            target = lax.div(owner * Ds, Dt)
            columns = pl.ds(pl.multiple_of(lax.rem(owner * Ds, Dt), 128), Ds)
            PART[layer, target, :, columns] = jnp.dot(
                MIX[...], WO[layer, owner], preferred_element_type=F32
            ).astype(BF16)
            if S == T:
                at = lax.div(target, 2)

                @pl.when(lax.rem(target, 2) != core)
                def _():
                    pair_copy(layer, at).start()

                @pl.when(jnp.logical_and(lax.rem(target, 2) == core, at != chip))
                def _():
                    sum_pair(layer, at)

        by_arrival(block)
        if S != T:
            for shift in list(range(1, chips)) + [0]:
                pair_copy(layer, lax.rem(chip + shift, chips)).start()
            for shift in range(1, chips):
                sum_pair(layer, lax.rem(chip + shift, chips))

    def finish(layer):
        pair_copy(layer, chip).wait_recv()
        for shift in range(1, chips):
            sum_arrival(layer, lax.rem(chip + shift, chips)).wait_recv()
        source = h_ref if layer == 0 else HB
        target = out_ref if layer == L - 1 else HB

        def body(where):
            total = PART[layer, t, where, :].astype(F32) + PRECV[layer, chip, where, :].astype(F32)
            for shift in range(1, chips):
                total = total + RECV[layer, lax.rem(chip + shift, chips), where, :].astype(F32)
            target[where, :] = (source[where, :].astype(F32) + total).astype(BF16)

        each_chunk(body)

    barrier = pltpu.get_barrier_semaphore()
    for shift in range(1, T):
        pl.semaphore_signal(barrier, inc=1, device_id={"tp": lax.rem(t + shift, T)}, device_id_type=MESH)
    pl.semaphore_signal(barrier, inc=1, device_id={"grp": 1 - g}, device_id_type=MESH)

    @pl.when(jnp.logical_not(first))
    def _():
        pl.semaphore_signal(barrier, inc=1, device_id={"sp": me - 1}, device_id_type=MESH)

    @pl.when(jnp.logical_not(last))
    def _():
        pl.semaphore_signal(barrier, inc=1, device_id={"sp": me + 1}, device_id_type=MESH)

    inner = jnp.where(first, 0, 1) + jnp.where(last, 0, 1)
    pl.semaphore_wait(barrier, T + inner)

    event(0, 0)
    event(1, 0)
    make_x(0)
    send_x(0)

    def pumped(items, stages, start=1):
        for k in range(start, S):
            for item in items:
                event(item, k)
            if stages:
                stages.pop(0)()
        for stage in stages:
            stage()

    stages = [functools.partial(relay_x, 0), functools.partial(wait_x, 0)]
    ahead = 1
    for layer in range(L):
        base = 4 * layer
        if ahead > 1:
            event(base + 1, 1)
        pumped([base, base + 1], stages, ahead)
        event(base + 2, 0)
        event(base + 3, 0)
        event(base + 2, 1)
        event(base + 3, 1)
        if layer + 1 < L:
            event(base + 4, 0)
        project(layer)
        gate(layer)
        pumped(
            [base + 2, base + 3],
            [functools.partial(convolve, layer), functools.partial(mix, layer)],
            2,
        )
        if layer + 1 < L:
            event(base + 5, 0)
            event(base + 4, 1)
            ahead = 2
        branch(layer)
        if layer + 1 < L:

            def next_x(layer=layer):
                finish(layer)
                make_x(layer + 1)
                send_x(layer + 1)

            def arrive_x(layer=layer):
                relay_x(layer + 1)
                wait_x(layer + 1)

            stages = [next_x, arrive_x]
        else:
            finish(layer)

    for item in range(4 * L):

        def drain(owner, _, item=item):
            @pl.when(jnp.logical_and(owner <= me, jnp.logical_not(last)))
            def _():
                zcopy(item, owner, 1).wait_send()

            @pl.when(jnp.logical_and(owner >= me, jnp.logical_not(first)))
            def _():
                zcopy(item, owner, -1).wait_send()

            @pl.when(owner != me)
            def _():
                ycopy(item, owner).wait_send()

            return 0

        lax.fori_loop(0, S, drain, 0)
    for layer in range(L):
        for slot in (2 * layer, 2 * layer + 1):
            for shift in range(1, T):
                stat_copy(slot, lax.rem(t + shift, T)).wait_send()
        for shift in range(chips):
            xcopy(layer, t, partner, xs.at[layer, shift]).wait_send()
            pair_copy(layer, lax.rem(chip + shift, chips)).wait_send()
        for shift in range(1, chips):
            xcopy(layer, t, partner, xf.at[layer, shift]).wait_send()
            sum_copy(layer, lax.rem(chip + shift, chips)).wait_send()

        @pl.when(jnp.logical_not(last))
        def _(layer=layer):
            halo_copy(layer).wait_send()


def shards(hidden_in, in_gain, w_value, w_gate, conv_taps, norm_gain, norm_shift, w_out):
    S, T = lax.axis_size("sp"), lax.axis_size("tp")
    L, Ds, Cn = w_value.shape
    rows, Dt = hidden_in.shape
    chips = T // 2
    halo = (conv_taps.shape[1] - 1 + 7) // 8 * 8
    vmem = pl.BlockSpec(memory_space=pltpu.VMEM)
    hbm = pl.BlockSpec(memory_space=pl.ANY)
    dma = pltpu.SemaphoreType.DMA
    return pl.pallas_call(
        functools.partial(kernel, S, T),
        out_shape=jax.ShapeDtypeStruct((rows, Dt), BF16),
        in_specs=[vmem, vmem, hbm, hbm, vmem, vmem, vmem, hbm],
        out_specs=vmem,
        scratch_shapes=[
            pltpu.VMEM((L, S, Ds, Cn), BF16),
            pltpu.VMEM((L, S, Ds, Cn), BF16),
            pltpu.VMEM((L, S, Cn, Ds), BF16),
            pltpu.VMEM((L, T, rows, Dt), BF16),
            pltpu.VMEM((2, rows, Cn), F32),
            pltpu.VMEM((L, rows + halo, Cn), F32),
            pltpu.VMEM((rows, Cn), F32),
            pltpu.VMEM((rows, Cn), BF16),
            pltpu.VMEM((L, T, rows, Dt), BF16),
            pltpu.VMEM((L, chips, rows, Dt), BF16),
            pltpu.VMEM((L, chips, rows, Dt), BF16),
            pltpu.VMEM((L, chips, rows, Dt), BF16),
            pltpu.VMEM((2 * L, T, 8, rows), F32),
            pltpu.VMEM((rows, Dt), BF16),
            dma((L, 3)),
            dma((4 * L, S)), dma((4 * L, S)), dma((4 * L, S)), dma((4 * L, S)), dma((4 * L, S)),
            dma((L, T)), dma((L, chips)), dma((L, chips)),
            dma((2 * L, T)), dma((2 * L, T)),
            dma((L,)), dma((L,)),
            dma((L, chips)), dma((L, chips)),
            dma((L, chips)), dma((L, chips)),
        ],
        compiler_params=pltpu.CompilerParams(
            collective_id=0, has_side_effects=True, vmem_limit_bytes=64_000_000
        ),
    )(hidden_in, in_gain, w_value, w_gate, conv_taps, norm_gain, norm_shift, w_out)


def solution(mesh):
    placed = (
        P(("grp", "sp"), "tp"),
        P(None, "tp"),
        P(None, "sp", "tp"),
        P(None, "sp", "tp"),
        P(None, None, "tp"),
        P(None, "tp"),
        P(None, "tp"),
        P(None, "tp", "sp"),
    )
    return jax.shard_map(
        shards, mesh=mesh, in_specs=placed, out_specs=P(("grp", "sp"), "tp"), check_vma=False
    )
```
